32 devices in a mesh: sp: 32 (over z, y, x, core), tp: 1.
Axes of the slice: x: 2, y: 2, z: 4, core: 2. Of those that a mesh axis runs over, the one named last changes fastest.
Arguments:
- queries: bfloat16 [8192, 1024], P('sp', 'tp'), may hold values from -30 to 30
- keys: bfloat16 [8192, 256], P('sp', 'tp'), may hold values from -30 to 30
- values: bfloat16 [8192, 256], P('sp', 'tp'), may hold values from -20 to 20
- gate_totals: float32 [8192, 16], P('sp', 'tp'), may hold values from -8192 to 0, as said below
- documents: int32 [8192], P('sp'), may hold values from 0 to 1, never falling along the last dimension, each value on 1 to 6144 neighbouring positions
- stream: bfloat16 [8192, 2048], P(('sp', 'tp')), may hold values from -3 to 3
- out_weight: bfloat16 [1024, 2048], replicated, may hold values from -0.1875 to 0.1875
- norm_gain: float32 [2048], replicated, may hold values from 0.1 to 1.9
- routes: int32 [8192, 2], P(('sp', 'tp')), may hold values from 0 to 31, all different within a row; in each aligned block of 256 rows (0 to 255, 256 to 511, ...) at most 32 rows name the same one
- route_weights: float32 [8192, 2], P(('sp', 'tp')), may hold values from 0.2 to 1
- expert_gate: bfloat16 [32, 2048, 1024], P('sp', None, 'tp'), may hold values from -0.125 to 0.125
- expert_up: bfloat16 [32, 2048, 1024], P('sp', None, 'tp'), may hold values from -0.125 to 0.125
- expert_down: bfloat16 [32, 1024, 2048], P('sp', 'tp'), may hold values from -0.1875 to 0.1875
Outputs:
- output: bfloat16 [8192, 2048], P(('sp', 'tp'))
The draws below stay inside these ranges and needn't reach their ends.
Inputs may be any that keep to these rules, and one draw needn't show every extreme that they name: `gate_totals`: along positions it never rises, for every head. `routes`: in each aligned block of rows held by one device, no expert is named by more than 32 rows.
All inputs are finite; a program needn't handle non-finite values.
Results may differ from the reference program's by a relative error of at most 0.014.
Values may be sent and summed in bfloat16 or wider, within the bound.
A program may use at most 128 MiB of HBM per device.

```python
import math
import jax
import jax.numpy as jnp
import numpy as np
from jax import lax

D = 2048
QUERY_HEAD_COUNT = 16
KV_HEADS = 4
HD = 64
FF = 1024
TOP = 2
DOCS = 2
TOK_DEV = 256
SEQUENCE_TOKENS = 8192
EXPERTS = 32
CAP = 32
DOC_MOST = 6144
N_SP = 32
N_TP = 1


def draw_keys(key, part):
    base = jax.random.normal(jax.random.fold_in(key, 2), (SEQUENCE_TOKENS, KV_HEADS, HD), jnp.float32)
    return base.reshape(SEQUENCE_TOKENS, KV_HEADS * HD).astype(jnp.bfloat16)


def draw_queries(key, part):
    group = QUERY_HEAD_COUNT // KV_HEADS
    base = jax.random.normal(jax.random.fold_in(key, 1), (SEQUENCE_TOKENS, KV_HEADS, group, HD), jnp.float32)
    return base.reshape(SEQUENCE_TOKENS, QUERY_HEAD_COUNT * HD).astype(jnp.bfloat16)


def draw_gate_totals(key, part):
    ranking = jax.random.permutation(jax.random.fold_in(key, 21), QUERY_HEAD_COUNT)
    faster_variant = ranking < QUERY_HEAD_COUNT // 2
    slow_total = jax.random.uniform(jax.random.fold_in(key, 22), (QUERY_HEAD_COUNT,), jnp.float32, 0.15, 0.5)
    quick_rate = 1.0 / jax.random.uniform(jax.random.fold_in(key, 23), (QUERY_HEAD_COUNT,), jnp.float32, 30.0, 60.0)
    decay_speed = jnp.where(faster_variant, quick_rate, slow_total / SEQUENCE_TOKENS)
    machine_multiplier = jnp.exp(jax.random.uniform(jax.random.fold_in(key, 24), (SEQUENCE_TOKENS // TOK_DEV, 1), jnp.float32, -0.7, 0.7))
    machine_multiplier = jnp.repeat(machine_multiplier, TOK_DEV, axis=0)
    coarse_estimate = jax.random.uniform(jax.random.fold_in(key, 25), (SEQUENCE_TOKENS, QUERY_HEAD_COUNT), jnp.float32, 0.4, 1.6)
    cluster_positions = jax.random.randint(jax.random.fold_in(key, 26), (2, QUERY_HEAD_COUNT), 0, SEQUENCE_TOKENS)
    cluster_dropout = jnp.log(jax.random.uniform(jax.random.fold_in(key, 27), (2, QUERY_HEAD_COUNT), jnp.float32, 0.55, 0.8))
    locations = jnp.arange(SEQUENCE_TOKENS, dtype=jnp.int32)[:, None]
    token_clusters = jnp.where(locations == cluster_positions[0][None, :], cluster_dropout[0][None, :], 0.0)
    token_clusters = token_clusters + jnp.where(locations == cluster_positions[1][None, :], cluster_dropout[1][None, :], 0.0)
    logarithm_gate = -decay_speed[None, :] * machine_multiplier * coarse_estimate + jnp.where(faster_variant[None, :], 0.0, token_clusters)
    return jnp.cumsum(logarithm_gate, axis=0).astype(jnp.float32)


def shard_levels(rng, shape, shards, smallest, top_value):
    loudness = 1.0
    for axis_at, parts in shards:
        heights = jax.random.uniform(jax.random.fold_in(jax.random.fold_in(rng, 6), axis_at), (parts,), jnp.float32, smallest / len(shards), top_value / len(shards))
        loudness = loudness * jnp.repeat(jnp.exp(heights), shape[axis_at] // parts).reshape((-1,) + (1,) * (len(shape) - 1 - axis_at))
    return loudness


def length_profile(count, total, bound, slope):
    loads = [(1 << 20) // math.isqrt(grade ** slope) + 1 for grade in range(2, count + 1)]
    rest, counts = total - bound - (count - 1), [1] * (count - 1)
    while rest > 0:
        free = [i for i in range(count - 1) if counts[i] < bound]
        whole, remaining = sum([loads[i] for i in free]), rest
        for i in free:
            extra = min(bound - counts[i], max(1, remaining * loads[i] // whole), rest)
            counts[i] = counts[i] + extra
            rest = rest - extra
    return np.array([bound] + counts)


def ragged_sizes(stream_key, amount, total, most, slope):
    if amount == 2:
        one = jax.random.randint(stream_key, (), max(1, total - most), min(most, total - 1) + 1)
        return jnp.stack([one, total - one])
    tallies = jnp.asarray(length_profile(amount, total, most, slope), jnp.int32)
    twos = (amount - 1) // 2
    donor, receiver = tallies[1:1 + 2 * twos:2], tallies[2:2 + 2 * twos:2]
    slack = jnp.minimum(donor - 1, most - receiver)
    shifted = jax.random.randint(jax.random.fold_in(stream_key, 1), (twos,), 0, 1 << 20) % (slack + 1)
    tallies = tallies.at[1:1 + 2 * twos:2].set(donor - shifted).at[2:2 + 2 * twos:2].set(receiver + shifted)
    return tallies[jax.random.permutation(jax.random.fold_in(stream_key, 2), amount)]


def assign_block(own_key, own, number, rows, amount, top, most, slope):
    order = jax.random.permutation(own_key, amount)
    crowded, usual = portions_of(amount, rows * top, most, slope, True), portions_of(amount, rows * top, most, slope, False)
    places = jnp.arange(amount)

    def named(sizes, offset_by):
        used = int((sizes > 0).sum())
        fixed = max(1, used // 4)
        passed = fixed + (places - fixed + offset_by * (used - fixed)) % max(1, amount - fixed)
        return jnp.zeros((amount,), jnp.int32).at[order[jnp.where(places < fixed, places, passed)]].set(jnp.asarray(sizes, jnp.int32))

    sizes = jnp.where(number % 4 == 0, named(crowded, number // 4), named(usual, number - number // 4 - 1))
    mixed = jax.random.permutation(jax.random.fold_in(own, 3), amount)
    donor, taker = mixed[0:amount // 2 * 2:2], mixed[1:amount // 2 * 2:2]
    slack = jnp.minimum(sizes[donor] - 1, most - sizes[taker]) // 2
    slack = jnp.where((donor == order[0]) | (taker == order[0]) | (sizes[taker] == 0), 0, jnp.maximum(slack, 0))
    passed = jax.random.randint(jax.random.fold_in(own, 4), (amount // 2,), 0, 1 << 20) % (slack + 1)
    sizes = sizes.at[donor].add(-passed).at[taker].add(passed)
    labels = jnp.searchsorted(jnp.cumsum(sizes), jnp.arange(rows * top), side="right").astype(jnp.int32)
    table = labels.reshape(top, rows).T
    table = table[jax.random.permutation(jax.random.fold_in(own, 1), rows)]
    offset_by = jax.random.randint(jax.random.fold_in(own, 2), (rows, 1), 0, top)
    return jnp.take_along_axis(table, (jnp.arange(top)[None, :] + offset_by) % top, axis=1)


def portions_of(amount, total, bound, slope, full):
    weights = [(1 << 20) // math.isqrt(standing ** slope) + 1 for standing in range(1, amount + 1)]
    largest = bound if full else min(bound, max(-(-total // amount), total * weights[0] // sum(weights)))
    least = 1 if total - largest >= amount - 1 else 0
    counts, spare = [largest] + [least] * (amount - 1), total - largest - least * (amount - 1)
    while spare > 0:
        free = [i for i in range(1, amount) if counts[i] < largest] or [i for i in range(1, amount) if counts[i] < bound]
        whole, budget = sum([weights[i] for i in free]), spare
        for i in free:
            more = min(bound - counts[i], max(1, budget * weights[i] // whole), spare)
            counts[i] = counts[i] + more
            spare = spare - more
    return np.array(counts)


def normal_values(key, extent, deviation, reach, split=(), kind=jnp.bfloat16):
    values = jax.random.normal(key, extent, jnp.float32) * deviation
    if len(split) > 0:
        values = shard_levels(key, extent, split, -0.22, 0.18) * values
    return jnp.clip(values, min=-reach, max=reach).astype(kind)


def setup_inputs(seed: int = 0) -> dict:
    splits = jax.random.split(jax.random.key(seed), 14)
    queries = draw_queries(jax.random.fold_in(splits[13], 71), 0)
    keys = draw_keys(jax.random.fold_in(splits[13], 71), 0)
    values = normal_values(splits[2], (SEQUENCE_TOKENS, KV_HEADS * HD), 4.0, 20.0, ((0, 32),))
    gate_totals = draw_gate_totals(jax.random.fold_in(splits[13], 71), 0)
    documents = jnp.searchsorted(jnp.cumsum(ragged_sizes(splits[4], DOCS, SEQUENCE_TOKENS, DOC_MOST, 1)), jnp.arange(SEQUENCE_TOKENS), side="right").astype(jnp.int32)
    stream = normal_values(splits[5], (SEQUENCE_TOKENS, D), 0.5, 3.0, ((0, 32),))
    out_weight = normal_values(splits[6], (QUERY_HEAD_COUNT * HD, D), (QUERY_HEAD_COUNT * HD) ** -0.5, 0.1875)
    norm_gain = jnp.clip(1.0 + 0.18 * jax.random.normal(splits[7], (D,), jnp.float32), 0.1, 1.9)
    routes_keys = jax.random.split(jax.random.fold_in(splits[8], 1), SEQUENCE_TOKENS // (TOK_DEV // N_TP))
    routes_turns = jax.random.permutation(jax.random.fold_in(splits[8], 3), SEQUENCE_TOKENS // (TOK_DEV // N_TP))
    routes = jax.vmap(lambda own, number: assign_block(jax.random.fold_in(splits[8], 2), own, number, TOK_DEV // N_TP, EXPERTS, TOP, CAP, 1))(routes_keys, routes_turns).reshape((SEQUENCE_TOKENS, TOP))
    route_weights = jnp.clip(0.2 + 0.8 * jax.random.uniform(splits[9], (SEQUENCE_TOKENS, TOP), jnp.float32) ** shard_levels(splits[9], (SEQUENCE_TOKENS, TOP), ((0, 32),), -0.2, 0.2), 0.2, 1.0)
    expert_gate = normal_values(splits[10], (EXPERTS, D, FF), D ** -0.5, 0.125, ((0, 32),))
    expert_up = normal_values(splits[11], (EXPERTS, D, FF), D ** -0.5, 0.125, ((0, 32),))
    expert_down = normal_values(splits[12], (EXPERTS, FF, D), FF ** -0.5, 0.1875, ((0, 32),))
    return {"queries": queries, "keys": keys, "values": values, "gate_totals": gate_totals, "documents": documents, "stream": stream, "out_weight": out_weight, "norm_gain": norm_gain, "routes": routes, "route_weights": route_weights, "expert_gate": expert_gate, "expert_up": expert_up, "expert_down": expert_down}


EPS = 1e-06
MASKED = -1e+30

def attend(queries, keys, values, gate_totals, documents):
    group = QUERY_HEAD_COUNT // KV_HEADS
    block = min(256, SEQUENCE_TOKENS)
    scale = HD ** (-0.5)
    key_all = keys.astype(jnp.float32).reshape(SEQUENCE_TOKENS, KV_HEADS, HD)
    value_all = values.astype(jnp.float32).reshape(SEQUENCE_TOKENS, KV_HEADS, HD)
    key_gate = gate_totals.T.reshape(KV_HEADS, group, 1, SEQUENCE_TOKENS)
    key_pos = jnp.arange(SEQUENCE_TOKENS, dtype=jnp.int32)

    def one_block(index):
        start = (index * block).astype(jnp.int32)
        query_blk = lax.dynamic_slice_in_dim(queries, start, block, 0).astype(jnp.float32).reshape(block, KV_HEADS, group, HD)
        query_gate = lax.dynamic_slice_in_dim(gate_totals, start, block, 0).T.reshape(KV_HEADS, group, block, 1)
        query_doc = lax.dynamic_slice_in_dim(documents, start, block, 0)
        query_pos = start + jnp.arange(block, dtype=jnp.int32)
        scores = jnp.einsum('qkgd,skd->kgqs', query_blk, key_all) * scale + query_gate - key_gate
        allowed = (key_pos[None, :] <= query_pos[:, None]) & (documents[None, :] == query_doc[:, None])
        scores = jnp.where(allowed, scores, MASKED)
        highest = lax.optimization_barrier(jnp.max(scores, axis=-1, keepdims=True))
        weights = jnp.where(allowed, jnp.exp(scores - highest), 0.0)
        totals = lax.optimization_barrier(jnp.sum(weights, axis=-1))
        rounded = lax.optimization_barrier(weights.astype(jnp.bfloat16)).astype(jnp.float32)
        mixed = jnp.einsum('kgqs,skd->kgqd', rounded, value_all) / totals[..., None]
        return jnp.transpose(mixed, (2, 0, 1, 3)).reshape(block, QUERY_HEAD_COUNT * HD).astype(jnp.bfloat16)
    blocks = lax.map(one_block, jnp.arange(SEQUENCE_TOKENS // block, dtype=jnp.int32))
    return blocks.reshape(SEQUENCE_TOKENS, QUERY_HEAD_COUNT * HD)

def run_experts(normed, routes, expert_gate, expert_up, expert_down):
    flat = routes.reshape(-1)
    load = N_SP * N_TP * CAP
    half = FF // N_TP

    def one_expert(expert):
        rank_key = jnp.where(flat == expert, 0, 1).astype(jnp.int32)
        order = jnp.argsort(rank_key, stable=True)[:load].astype(jnp.int32)
        valid = flat[order] == expert
        picked = normed[order // TOP]
        gate = jnp.dot(picked, expert_gate[expert], preferred_element_type=jnp.float32)
        upper = jnp.dot(picked, expert_up[expert], preferred_element_type=jnp.float32)
        inner = (jax.nn.silu(gate) * upper).astype(jnp.bfloat16)
        answer = jnp.zeros((load, D), jnp.float32)
        for portion in range(N_TP):
            piece = jnp.dot(inner[:, portion * half:(portion + 1) * half], expert_down[expert][portion * half:(portion + 1) * half], preferred_element_type=jnp.float32)
            answer = answer + lax.optimization_barrier(piece.astype(jnp.bfloat16)).astype(jnp.float32)
        answer = jnp.where(valid[:, None], answer.astype(jnp.bfloat16).astype(jnp.float32), 0.0)
        return (order, answer)
    orders, answers = lax.map(one_expert, jnp.arange(EXPERTS, dtype=jnp.int32))
    entries = jnp.zeros((flat.shape[0], D), jnp.float32).at[orders.reshape(-1)].add(answers.reshape(-1, D))
    return entries.reshape(SEQUENCE_TOKENS, TOP, D)

def reference(queries, keys, values, gate_totals, documents, stream, out_weight, norm_gain, routes, route_weights, expert_gate, expert_up, expert_down):
    attended = attend(queries, keys, values, gate_totals, documents)
    hidden = (stream.astype(jnp.float32) + jnp.dot(attended, out_weight, preferred_element_type=jnp.float32)).astype(jnp.bfloat16)
    hidden_f = hidden.astype(jnp.float32)
    normed = (hidden_f * lax.rsqrt(lax.optimization_barrier(jnp.mean(hidden_f * hidden_f, axis=-1, keepdims=True)) + EPS) * norm_gain).astype(jnp.bfloat16)
    entries = run_experts(normed, routes, expert_gate, expert_up, expert_down)
    routed = lax.optimization_barrier(jnp.sum(route_weights[..., None] * entries, axis=1))
    return (hidden_f + routed).astype(jnp.bfloat16)
```

```python
import functools
import math

import jax
import jax.numpy as jnp
from jax import lax
from jax.experimental import pallas as pl
from jax.experimental.pallas import tpu as pltpu
from jax.sharding import PartitionSpec as P

QUERY_HEAD_COUNT = 16
KV_HEADS = 4
HD = 64
TOP = 2


EPS = 1e-06
MASKED = -1e30


def make_fold(query_rows, query_gate, key_gate_all, query_docs, first_pos, kv_local, group):
    count = query_rows.shape[0]
    scale = HD ** (-0.5)
    query_blk = query_rows.reshape(count, kv_local, group, HD)
    gate_here = query_gate.T.reshape(kv_local, group, count, 1)
    query_pos = first_pos + jnp.arange(count, dtype=jnp.int32)
    last_pos = first_pos + count - 1
    first_doc = query_docs[0]

    def block_step(carry, block_in):
        running_max, running_sum, carried = carry
        key_block, value_block, doc_block, pos_block = block_in
        width = key_block.shape[0]

        def compute(unused):
            key_heads = key_block.reshape(width, kv_local, HD)
            value_heads = value_block.reshape(width, kv_local, HD)
            gate_keys = lax.dynamic_slice_in_dim(key_gate_all, pos_block[0], width, 0).T.reshape(
                kv_local, group, 1, width
            )
            scores = (
                jnp.einsum(
                    "qkgd,nkd->kgqn", query_blk, key_heads, preferred_element_type=jnp.float32
                )
                * scale
                + gate_here
                - gate_keys
            )
            allowed = (pos_block[None, :] <= query_pos[:, None]) & (
                doc_block[None, :] == query_docs[:, None]
            )
            scores = jnp.where(allowed, scores, MASKED)
            new_max = jnp.maximum(running_max, jnp.max(scores, axis=-1))
            weights = jnp.where(allowed, jnp.exp(scores - new_max[..., None]), 0.0)
            factor = jnp.exp(running_max - new_max)
            new_sum = running_sum * factor + jnp.sum(weights, axis=-1)
            new_carried = carried * factor[..., None] + jnp.einsum(
                "kgqn,nkd->kgqd",
                weights.astype(jnp.bfloat16),
                value_heads,
                preferred_element_type=jnp.float32,
            )
            return (new_max, new_sum, new_carried)

        skipped = (pos_block[0] > last_pos) | (doc_block[width - 1] < first_doc)
        return (lax.cond(skipped, lambda unused: carry, compute, 0), None)

    def fold(carry, piece, start):
        key_piece, value_piece, doc_piece = piece
        length = key_piece.shape[0]
        width = math.gcd(length, 512)
        blocks_count = length // width
        pos_piece = jnp.arange(length, dtype=jnp.int32)
        blocks = (
            key_piece.reshape(blocks_count, width, -1),
            value_piece.reshape(blocks_count, width, -1),
            doc_piece.reshape(blocks_count, width),
            pos_piece.reshape(blocks_count, width),
        )
        carry, unused = lax.scan(block_step, carry, blocks)
        return carry

    initial = (
        jnp.full((kv_local, group, count), MASKED, jnp.float32),
        jnp.zeros((kv_local, group, count), jnp.float32),
        jnp.zeros((kv_local, group, count, HD), jnp.float32),
    )
    return (fold, initial)


def finish(running_sum, carried):
    mixed = carried / running_sum[..., None]
    count = mixed.shape[2]
    return jnp.transpose(mixed, (2, 0, 1, 3)).reshape(count, -1).astype(jnp.bfloat16)


def shards(
    queries,
    keys,
    values,
    gate_totals,
    documents,
    stream,
    out_weight,
    norm_gain,
    routes,
    route_weights,
    expert_gate,
    expert_up,
    expert_down,
):
    tp_count = lax.axis_size("tp")
    sp_count = lax.axis_size("sp")
    tp_index = lax.axis_index("tp")
    sp_index = lax.axis_index("sp")
    group = QUERY_HEAD_COUNT // KV_HEADS
    tok_local = queries.shape[0]
    own_rows = tok_local // tp_count
    first_row = sp_index * tok_local
    query_rows = lax.all_to_all(queries, "tp", split_axis=0, concat_axis=1, tiled=True)
    key_whole, value_whole = (
        lax.all_gather(keys, "tp", axis=1, tiled=True),
        lax.all_gather(values, "tp", axis=1, tiled=True),
    )
    gate_whole = lax.all_gather(gate_totals, "tp", axis=1, tiled=True)
    key_gate_all = lax.all_gather(gate_whole, "sp", axis=0, tiled=True)
    query_gate = lax.dynamic_slice_in_dim(gate_whole, tp_index * own_rows, own_rows, 0)
    query_docs = lax.dynamic_slice_in_dim(documents, tp_index * own_rows, own_rows, 0)
    fold, initial = make_fold(
        query_rows,
        query_gate,
        key_gate_all,
        query_docs,
        first_row + tp_index * own_rows,
        KV_HEADS,
        group,
    )
    running_max, running_sum, carried = fold(
        initial,
        (
            lax.all_gather(key_whole, "sp", axis=0, tiled=True),
            lax.all_gather(value_whole, "sp", axis=0, tiled=True),
            lax.all_gather(documents, "sp", axis=0, tiled=True),
        ),
        jnp.int32(0),
    )
    attended = finish(running_sum, carried)
    hidden = (
        stream.astype(jnp.float32)
        + jnp.dot(attended, out_weight, preferred_element_type=jnp.float32)
    ).astype(jnp.bfloat16)
    hidden_f = hidden.astype(jnp.float32)
    normed = (
        hidden_f
        * lax.rsqrt(jnp.mean(hidden_f * hidden_f, axis=-1, keepdims=True) + EPS)
        * norm_gain
    ).astype(jnp.bfloat16)
    local_experts = expert_gate.shape[0]
    experts_total = local_experts * sp_count
    capacity = max(2, 2 * tok_local * TOP // (tp_count * experts_total))
    flat = routes.reshape(-1)
    hits = (flat[:, None] == jnp.arange(experts_total, dtype=jnp.int32)[None, :]).astype(jnp.int32)
    slot_index = jnp.sum(jnp.cumsum(hits, axis=0) * hits, axis=1) - 1
    target = flat * capacity + slot_index
    entry_rows = jnp.repeat(normed, TOP, axis=0)
    outgoing = (
        jnp.zeros((experts_total * capacity, normed.shape[1]), jnp.bfloat16)
        .at[target]
        .set(entry_rows)
    )
    outgoing = outgoing.reshape(experts_total, capacity, -1)
    arrived = lax.all_to_all(outgoing, "sp", split_axis=0, concat_axis=0, tiled=True)
    slots = arrived.shape[1]
    both_halves = lax.all_gather(arrived, "tp", axis=0, tiled=True)
    grouped = both_halves.reshape(tp_count * sp_count, local_experts, slots, -1)
    gate = jnp.einsum("secd,edf->secf", grouped, expert_gate, preferred_element_type=jnp.float32)
    upper = jnp.einsum("secd,edf->secf", grouped, expert_up, preferred_element_type=jnp.float32)
    inner = (jax.nn.silu(gate) * upper).astype(jnp.bfloat16)
    partial_value = jnp.einsum(
        "secf,efd->secd", inner, expert_down, preferred_element_type=jnp.float32
    )
    partial_value = lax.optimization_barrier(partial_value.astype(jnp.bfloat16)).astype(jnp.float32)
    summed = lax.psum_scatter(
        partial_value.reshape(tp_count * sp_count * local_experts, slots, -1).astype(jnp.bfloat16),
        "tp",
        scatter_dimension=0,
        tiled=True,
    )
    returned = lax.all_to_all(summed, "sp", split_axis=0, concat_axis=0, tiled=True)
    answers = returned.reshape(experts_total * capacity, -1)[target].reshape(own_rows, TOP, -1)
    routed = jnp.sum(route_weights[..., None] * answers.astype(jnp.float32), axis=1)
    return (hidden_f + routed).astype(jnp.bfloat16)


def attend_kernel(sub, span, boundary_ref, query_ref, kv_ref, gate_ref, out_ref):
    tile = pl.program_id(0)
    stripes = kv_ref.shape[0]
    stripe = lax.rem(lax.axis_index("sp"), stripes)
    blocks = query_ref.shape[0]
    block = span // blocks
    group = QUERY_HEAD_COUNT // KV_HEADS
    rows = blocks * sub
    boundary = boundary_ref[0]
    first = tile * span
    heads = []
    zeros = jnp.zeros((rows, HD), jnp.bfloat16)
    query = query_ref[...].reshape(rows, group * HD) * jnp.bfloat16(HD ** (-0.5))
    for head in range(group):
        heads.append(jnp.concatenate([query[:, head * HD:(head + 1) * HD], zeros], axis=1))
    row = lax.broadcasted_iota(jnp.int32, (rows, 1), 0)
    query_pos = first + (row // sub) * block + stripe * sub + lax.rem(row, sub)
    doc_start = jnp.where(query_pos >= boundary, boundary, 0)

    def chunk(index, carry, masked):
        per_z = stripes // blocks
        kv = kv_ref[pl.ds(lax.rem(index, per_z) * blocks, blocks), index // per_z, 0:block, :]
        kv = kv.reshape(span, 2 * HD)
        gates = gate_ref[index]
        origin = gate_ref[tile][:, 0:1]
        bias = origin - gates
        if masked:
            key_pos = index * span + lax.broadcasted_iota(jnp.int32, (1, span), 1)
            allowed = (key_pos <= query_pos) & (key_pos >= doc_start)
        result = []
        for head in range(group):
            top, total, mixed = carry[head]
            score = lax.dot_general(
                heads[head], kv, (((1,), (1,)), ((), ())), preferred_element_type=jnp.float32
            )
            score = score + bias[head:head + 1, :]
            if masked:
                score = jnp.where(allowed, score, MASKED)
            new_top = jnp.maximum(top, jnp.max(score, axis=1, keepdims=True))
            weight = jnp.exp(score - new_top)
            factor = jnp.exp(top - new_top)
            total = total * factor + jnp.sum(weight, axis=1, keepdims=True)
            mixed = mixed * factor + jnp.dot(
                weight.astype(jnp.bfloat16), kv, preferred_element_type=jnp.float32
            )
            result.append((new_top, total, mixed))
        return tuple(result)

    carry = tuple(
        (
            jnp.full((rows, 1), 0.5 * MASKED, jnp.float32),
            jnp.zeros((rows, 1), jnp.float32),
            jnp.zeros((rows, 2 * HD), jnp.float32),
        )
        for unused in range(group)
    )
    low = jnp.where(first >= boundary, boundary // span, 0)
    inside = (boundary > first) & (boundary < first + span)
    clean_low = jnp.where(inside, tile, jnp.where(first >= boundary, (boundary + span - 1) // span, 0))
    clean_low = jnp.minimum(clean_low, tile)
    carry = lax.fori_loop(low, clean_low, lambda i, c: chunk(i, c, True), carry)
    carry = lax.fori_loop(clean_low, tile, lambda i, c: chunk(i, c, False), carry)
    carry = chunk(tile, carry, True)
    parts = [mixed[:, HD:] / total for unused, total, mixed in carry]
    out_ref[...] = jnp.concatenate(parts, axis=1).astype(jnp.bfloat16).reshape(out_ref.shape)


def fast_shards(
    queries,
    keys,
    values,
    gate_totals,
    documents,
    stream,
    out_weight,
    norm_gain,
    routes,
    route_weights,
    expert_gate,
    expert_up,
    expert_down,
):
    sp_count = lax.axis_size("sp")
    group = QUERY_HEAD_COUNT // KV_HEADS
    tok = queries.shape[0]
    stripes = sp_count // KV_HEADS
    sub = tok // stripes
    blocks = 4
    span = blocks * tok
    tiles = sp_count // blocks
    lanes = 2 * HD
    part_a = lax.reduce_precision(gate_totals, 8, 7)
    rest = gate_totals - part_a
    part_b = lax.reduce_precision(rest, 8, 7)
    part_c = rest - part_b
    parts = jnp.stack([part_a, part_b, part_c], axis=0).astype(jnp.bfloat16)
    parts = jnp.transpose(parts.reshape(3, tok, KV_HEADS, group), (2, 0, 3, 1))
    parts = parts.reshape(KV_HEADS, 3 * group, tok)
    docs = jnp.broadcast_to(documents.astype(jnp.bfloat16)[None, None, :], (KV_HEADS, 4, tok))
    extra = jnp.concatenate([parts, docs], axis=1).reshape(KV_HEADS, -1, lanes)
    kv = jnp.concatenate(
        [keys.reshape(tok, KV_HEADS, HD), values.reshape(tok, KV_HEADS, HD)], axis=2
    )
    message = jnp.concatenate([jnp.transpose(kv, (1, 0, 2)), extra], axis=1)
    across = [[g * stripes + j for g in range(KV_HEADS)] for j in range(stripes)]
    within = [[g * stripes + j for j in range(stripes)] for g in range(KV_HEADS)]
    column = lax.all_to_all(
        message, "sp", split_axis=0, concat_axis=0, axis_index_groups=across, tiled=True
    )
    kv_all = lax.all_gather(column, "sp", axis=0, axis_index_groups=within)
    query_send = jnp.transpose(
        queries.reshape(stripes, sub, KV_HEADS, group * HD), (2, 0, 1, 3)
    ).reshape(sp_count, sub, group * HD)
    query_got = lax.all_to_all(query_send, "sp", split_axis=0, concat_axis=0, tiled=True)
    extra_all = jnp.transpose(kv_all[:, :, tok:, :], (1, 0, 2, 3)).reshape(sp_count, 16, tok)
    extra_all = extra_all.astype(jnp.float32)
    boundary = jnp.sum((extra_all[:, 3 * group, :] < 0.5).astype(jnp.int32)).reshape(1)
    gates = extra_all[:, :group] + extra_all[:, group:2 * group] + extra_all[:, 2 * group:3 * group]
    gates = jnp.transpose(gates.reshape(tiles, blocks, group, tok), (0, 2, 1, 3))
    gates = gates.reshape(tiles, group, span)
    mixed = pl.pallas_call(
        functools.partial(attend_kernel, sub, span),
        grid=(tiles,),
        in_specs=[
            pl.BlockSpec(memory_space=pltpu.SMEM),
            pl.BlockSpec((blocks, sub, group * HD), lambda i: (i, 0, 0)),
            pl.BlockSpec(kv_all.shape, lambda i: (0, 0, 0, 0)),
            pl.BlockSpec(gates.shape, lambda i: (0, 0, 0)),
        ],
        out_specs=pl.BlockSpec((blocks, sub, group * HD), lambda i: (i, 0, 0)),
        out_shape=jax.ShapeDtypeStruct((sp_count, sub, group * HD), jnp.bfloat16),
        compiler_params=pltpu.CompilerParams(vmem_limit_bytes=48 * 1024 * 1024),
        name="attend",
    )(boundary, query_got, kv_all, gates)
    back = lax.all_to_all(mixed, "sp", split_axis=0, concat_axis=0, tiled=True)
    attended = jnp.transpose(
        back.reshape(KV_HEADS, stripes, sub, group * HD), (1, 2, 0, 3)
    ).reshape(tok, QUERY_HEAD_COUNT * HD)
    hidden = (
        stream.astype(jnp.float32)
        + jnp.dot(attended, out_weight, preferred_element_type=jnp.float32)
    ).astype(jnp.bfloat16)
    hidden_f = hidden.astype(jnp.float32)
    normed = (
        hidden_f
        * lax.rsqrt(jnp.mean(hidden_f * hidden_f, axis=-1, keepdims=True) + EPS)
        * norm_gain
    ).astype(jnp.bfloat16)
    experts_total = sp_count
    capacity = max(2, 2 * tok * TOP // experts_total)
    slots = experts_total * capacity
    flat = routes.reshape(-1)
    hits = (flat[:, None] == jnp.arange(experts_total, dtype=jnp.int32)[None, :]).astype(jnp.int32)
    slot_index = jnp.sum(jnp.cumsum(hits, axis=0) * hits, axis=1) - 1
    target = (flat * capacity + slot_index).reshape(tok, TOP)
    line = jnp.arange(slots, dtype=jnp.int32)
    placed = sum(
        (line[:, None] == target[:, k][None, :]).astype(jnp.bfloat16) for k in range(TOP)
    )
    outgoing = jnp.dot(placed, normed, preferred_element_type=jnp.float32).astype(jnp.bfloat16)
    arrived = lax.all_to_all(
        outgoing.reshape(experts_total, capacity, -1), "sp", split_axis=0, concat_axis=0, tiled=True
    ).reshape(slots, -1)
    gate = jnp.dot(arrived, expert_gate[0], preferred_element_type=jnp.float32)
    upper = jnp.dot(arrived, expert_up[0], preferred_element_type=jnp.float32)
    inner = (jax.nn.silu(gate) * upper).astype(jnp.bfloat16)
    answer = jnp.dot(inner, expert_down[0], preferred_element_type=jnp.float32).astype(jnp.bfloat16)
    returned = lax.all_to_all(
        answer.reshape(sp_count, capacity, -1), "sp", split_axis=0, concat_axis=0, tiled=True
    ).reshape(slots, -1)
    share = sum(
        jnp.where(line[None, :] == target[:, k][:, None], route_weights[:, k][:, None], 0.0)
        for k in range(TOP)
    )
    share_high = lax.reduce_precision(share, 8, 7)
    share_low = (share - share_high).astype(jnp.bfloat16)
    routed = jnp.dot(
        share_high.astype(jnp.bfloat16), returned, preferred_element_type=jnp.float32
    ) + jnp.dot(share_low, returned, preferred_element_type=jnp.float32)
    return (hidden_f + routed).astype(jnp.bfloat16)


def solution(mesh):
    sp_count, tp_count = mesh.shape["sp"], mesh.shape["tp"]
    fast = tp_count == 1 and sp_count % 32 == 0
    return jax.shard_map(
        fast_shards if fast else shards,
        mesh=mesh,
        in_specs=(
            P("sp", "tp"),
            P("sp", "tp"),
            P("sp", "tp"),
            P("sp", "tp"),
            P("sp"),
            P(("sp", "tp"), None),
            P(),
            P(),
            P(("sp", "tp"), None),
            P(("sp", "tp"), None),
            P("sp", None, "tp"),
            P("sp", None, "tp"),
            P("sp", "tp", None),
        ),
        out_specs=P(("sp", "tp"), None),
        check_vma=False,
    )
```

```python
import functools
import math

import jax
import jax.numpy as jnp
from jax import lax
from jax.experimental import pallas as pl
from jax.experimental.pallas import tpu as pltpu
from jax.sharding import PartitionSpec as P

QUERY_HEAD_COUNT = 16
KV_HEADS = 4
HD = 64
TOP = 2


EPS = 1e-06
MASKED = -1e30


def make_fold(query_rows, query_gate, key_gate_all, query_docs, first_pos, kv_local, group):
    count = query_rows.shape[0]
    scale = HD ** (-0.5)
    query_blk = query_rows.reshape(count, kv_local, group, HD)
    gate_here = query_gate.T.reshape(kv_local, group, count, 1)
    query_pos = first_pos + jnp.arange(count, dtype=jnp.int32)
    last_pos = first_pos + count - 1
    first_doc = query_docs[0]

    def block_step(carry, block_in):
        running_max, running_sum, carried = carry
        key_block, value_block, doc_block, pos_block = block_in
        width = key_block.shape[0]

        def compute(unused):
            key_heads = key_block.reshape(width, kv_local, HD)
            value_heads = value_block.reshape(width, kv_local, HD)
            gate_keys = lax.dynamic_slice_in_dim(key_gate_all, pos_block[0], width, 0).T.reshape(
                kv_local, group, 1, width
            )
            scores = (
                jnp.einsum(
                    "qkgd,nkd->kgqn", query_blk, key_heads, preferred_element_type=jnp.float32
                )
                * scale
                + gate_here
                - gate_keys
            )
            allowed = (pos_block[None, :] <= query_pos[:, None]) & (
                doc_block[None, :] == query_docs[:, None]
            )
            scores = jnp.where(allowed, scores, MASKED)
            new_max = jnp.maximum(running_max, jnp.max(scores, axis=-1))
            weights = jnp.where(allowed, jnp.exp(scores - new_max[..., None]), 0.0)
            factor = jnp.exp(running_max - new_max)
            new_sum = running_sum * factor + jnp.sum(weights, axis=-1)
            new_carried = carried * factor[..., None] + jnp.einsum(
                "kgqn,nkd->kgqd",
                weights.astype(jnp.bfloat16),
                value_heads,
                preferred_element_type=jnp.float32,
            )
            return (new_max, new_sum, new_carried)

        skipped = (pos_block[0] > last_pos) | (doc_block[width - 1] < first_doc)
        return (lax.cond(skipped, lambda unused: carry, compute, 0), None)

    def fold(carry, piece, start):
        key_piece, value_piece, doc_piece = piece
        length = key_piece.shape[0]
        width = math.gcd(length, 512)
        blocks_count = length // width
        pos_piece = jnp.arange(length, dtype=jnp.int32)
        blocks = (
            key_piece.reshape(blocks_count, width, -1),
            value_piece.reshape(blocks_count, width, -1),
            doc_piece.reshape(blocks_count, width),
            pos_piece.reshape(blocks_count, width),
        )
        carry, unused = lax.scan(block_step, carry, blocks)
        return carry

    initial = (
        jnp.full((kv_local, group, count), MASKED, jnp.float32),
        jnp.zeros((kv_local, group, count), jnp.float32),
        jnp.zeros((kv_local, group, count, HD), jnp.float32),
    )
    return (fold, initial)


def finish(running_sum, carried):
    mixed = carried / running_sum[..., None]
    count = mixed.shape[2]
    return jnp.transpose(mixed, (2, 0, 1, 3)).reshape(count, -1).astype(jnp.bfloat16)


def shards(
    queries,
    keys,
    values,
    gate_totals,
    documents,
    stream,
    out_weight,
    norm_gain,
    routes,
    route_weights,
    expert_gate,
    expert_up,
    expert_down,
):
    tp_count = lax.axis_size("tp")
    sp_count = lax.axis_size("sp")
    tp_index = lax.axis_index("tp")
    sp_index = lax.axis_index("sp")
    group = QUERY_HEAD_COUNT // KV_HEADS
    tok_local = queries.shape[0]
    own_rows = tok_local // tp_count
    first_row = sp_index * tok_local
    query_rows = lax.all_to_all(queries, "tp", split_axis=0, concat_axis=1, tiled=True)
    key_whole, value_whole = (
        lax.all_gather(keys, "tp", axis=1, tiled=True),
        lax.all_gather(values, "tp", axis=1, tiled=True),
    )
    gate_whole = lax.all_gather(gate_totals, "tp", axis=1, tiled=True)
    key_gate_all = lax.all_gather(gate_whole, "sp", axis=0, tiled=True)
    query_gate = lax.dynamic_slice_in_dim(gate_whole, tp_index * own_rows, own_rows, 0)
    query_docs = lax.dynamic_slice_in_dim(documents, tp_index * own_rows, own_rows, 0)
    fold, initial = make_fold(
        query_rows,
        query_gate,
        key_gate_all,
        query_docs,
        first_row + tp_index * own_rows,
        KV_HEADS,
        group,
    )
    running_max, running_sum, carried = fold(
        initial,
        (
            lax.all_gather(key_whole, "sp", axis=0, tiled=True),
            lax.all_gather(value_whole, "sp", axis=0, tiled=True),
            lax.all_gather(documents, "sp", axis=0, tiled=True),
        ),
        jnp.int32(0),
    )
    attended = finish(running_sum, carried)
    hidden = (
        stream.astype(jnp.float32)
        + jnp.dot(attended, out_weight, preferred_element_type=jnp.float32)
    ).astype(jnp.bfloat16)
    hidden_f = hidden.astype(jnp.float32)
    normed = (
        hidden_f
        * lax.rsqrt(jnp.mean(hidden_f * hidden_f, axis=-1, keepdims=True) + EPS)
        * norm_gain
    ).astype(jnp.bfloat16)
    local_experts = expert_gate.shape[0]
    experts_total = local_experts * sp_count
    capacity = max(2, 2 * tok_local * TOP // (tp_count * experts_total))
    flat = routes.reshape(-1)
    hits = (flat[:, None] == jnp.arange(experts_total, dtype=jnp.int32)[None, :]).astype(jnp.int32)
    slot_index = jnp.sum(jnp.cumsum(hits, axis=0) * hits, axis=1) - 1
    target = flat * capacity + slot_index
    entry_rows = jnp.repeat(normed, TOP, axis=0)
    outgoing = (
        jnp.zeros((experts_total * capacity, normed.shape[1]), jnp.bfloat16)
        .at[target]
        .set(entry_rows)
    )
    outgoing = outgoing.reshape(experts_total, capacity, -1)
    arrived = lax.all_to_all(outgoing, "sp", split_axis=0, concat_axis=0, tiled=True)
    slots = arrived.shape[1]
    both_halves = lax.all_gather(arrived, "tp", axis=0, tiled=True)
    grouped = both_halves.reshape(tp_count * sp_count, local_experts, slots, -1)
    gate = jnp.einsum("secd,edf->secf", grouped, expert_gate, preferred_element_type=jnp.float32)
    upper = jnp.einsum("secd,edf->secf", grouped, expert_up, preferred_element_type=jnp.float32)
    inner = (jax.nn.silu(gate) * upper).astype(jnp.bfloat16)
    partial_value = jnp.einsum(
        "secf,efd->secd", inner, expert_down, preferred_element_type=jnp.float32
    )
    partial_value = lax.optimization_barrier(partial_value.astype(jnp.bfloat16)).astype(jnp.float32)
    summed = lax.psum_scatter(
        partial_value.reshape(tp_count * sp_count * local_experts, slots, -1).astype(jnp.bfloat16),
        "tp",
        scatter_dimension=0,
        tiled=True,
    )
    returned = lax.all_to_all(summed, "sp", split_axis=0, concat_axis=0, tiled=True)
    answers = returned.reshape(experts_total * capacity, -1)[target].reshape(own_rows, TOP, -1)
    routed = jnp.sum(route_weights[..., None] * answers.astype(jnp.float32), axis=1)
    return (hidden_f + routed).astype(jnp.bfloat16)


def attend_kernel(sub, span, width, boundary_ref, query_ref, kv_ref, gate_ref, out_ref):
    tile = pl.program_id(0)
    stripes = kv_ref.shape[0]
    stripe = lax.rem(lax.axis_index("sp"), stripes)
    blocks = query_ref.shape[0]
    block = span // blocks
    group = QUERY_HEAD_COUNT // KV_HEADS
    rows = blocks * sub
    boundary = boundary_ref[0]
    first = tile * span
    per_tile = span // width
    taken = width // block
    zeros = jnp.zeros((rows, HD), jnp.bfloat16)
    query = query_ref[...].reshape(rows, group * HD) * jnp.bfloat16(HD ** (-0.5))
    stacked = jnp.concatenate(
        [
            jnp.concatenate([query[:, head * HD:(head + 1) * HD], zeros], axis=1)
            for head in range(group)
        ],
        axis=0,
    )
    row = lax.broadcasted_iota(jnp.int32, (rows, 1), 0)
    query_pos = first + (row // sub) * block + stripe * sub + lax.rem(row, sub)
    doc_start = jnp.where(query_pos >= boundary, boundary, 0)
    origin = gate_ref[tile * per_tile][:, :, 0:1]
    lane = lax.broadcasted_iota(jnp.int32, (width, 2 * HD), 1)

    def chunk(index, carry, masked):
        per_z = stripes // taken
        kv = kv_ref[pl.ds(lax.rem(index, per_z) * taken, taken), index // per_z, 0:block, :]
        kv = kv.reshape(width, 2 * HD)
        bias = origin - gate_ref[index]
        if masked:
            key_pos = index * width + lax.broadcasted_iota(jnp.int32, (1, width), 1)
            allowed = (key_pos <= query_pos) & (key_pos >= doc_start)
        scores = lax.dot_general(
            stacked, kv, (((1,), (1,)), ((), ())), preferred_element_type=jnp.float32
        )
        tops, mixed = carry
        new_tops, factors, weights = [], [], []
        for head in range(group):
            score = scores[head * rows:(head + 1) * rows] + bias[head]
            if masked:
                score = jnp.where(allowed, score, MASKED)
            new_top = jnp.maximum(tops[head], jnp.max(score, axis=1, keepdims=True))
            weight = jnp.exp(score - new_top)
            factor = jnp.exp(tops[head] - new_top)
            new_tops.append(new_top)
            factors.append(factor)
            weights.append(weight.astype(jnp.bfloat16))
        mixed = mixed * jnp.concatenate(factors, axis=0) + jnp.dot(
            jnp.concatenate(weights, axis=0),
            jnp.where(lane < HD, jnp.bfloat16(1), kv),
            preferred_element_type=jnp.float32,
        )
        return (tuple(new_tops), mixed)

    carry = (
        tuple(jnp.full((rows, 1), 0.5 * MASKED, jnp.float32) for unused in range(group)),
        jnp.zeros((group * rows, 2 * HD), jnp.float32),
    )
    own = tile * per_tile
    inside = (boundary > first) & (boundary < first + span)
    second = first >= boundary
    low = jnp.where(second, boundary // width, 0)
    clean_low = jnp.where(inside, own, jnp.where(second, (boundary + width - 1) // width, 0))
    clean_low = jnp.minimum(clean_low, own)
    carry = lax.fori_loop(low, clean_low, lambda i, c: chunk(i, c, True), carry)
    carry = lax.fori_loop(clean_low, own, lambda i, c: chunk(i, c, False), carry)
    carry = lax.fori_loop(own, own + per_tile, lambda i, c: chunk(i, c, True), carry)
    unused, mixed = carry
    ratio = mixed[:, HD:] / mixed[:, :HD]
    parts = [ratio[head * rows:(head + 1) * rows] for head in range(group)]
    out_ref[...] = jnp.concatenate(parts, axis=1).astype(jnp.bfloat16).reshape(out_ref.shape)


def fast_shards(
    queries,
    keys,
    values,
    gate_totals,
    documents,
    stream,
    out_weight,
    norm_gain,
    routes,
    route_weights,
    expert_gate,
    expert_up,
    expert_down,
):
    sp_count = lax.axis_size("sp")
    group = QUERY_HEAD_COUNT // KV_HEADS
    tok = queries.shape[0]
    stripes = sp_count // KV_HEADS
    sub = tok // stripes
    blocks = 4
    span = blocks * tok
    width = min(span, 1024)
    tiles = sp_count // blocks
    lanes = 2 * HD
    part_a = lax.reduce_precision(gate_totals, 8, 7)
    rest = gate_totals - part_a
    part_b = lax.reduce_precision(rest, 8, 7)
    part_c = rest - part_b
    parts = jnp.stack([part_a, part_b, part_c], axis=0).astype(jnp.bfloat16)
    parts = jnp.transpose(parts.reshape(3, tok, KV_HEADS, group), (2, 0, 3, 1))
    parts = parts.reshape(KV_HEADS, 3 * group, tok)
    docs = jnp.broadcast_to(documents.astype(jnp.bfloat16)[None, None, :], (KV_HEADS, 4, tok))
    extra = jnp.concatenate([parts, docs], axis=1).reshape(KV_HEADS, -1, lanes)
    kv = jnp.concatenate(
        [keys.reshape(tok, KV_HEADS, HD), values.reshape(tok, KV_HEADS, HD)], axis=2
    )
    message = jnp.concatenate([jnp.transpose(kv, (1, 0, 2)), extra], axis=1)
    across = [[g * stripes + j for g in range(KV_HEADS)] for j in range(stripes)]
    within = [[g * stripes + j for j in range(stripes)] for g in range(KV_HEADS)]
    column = lax.all_to_all(
        message, "sp", split_axis=0, concat_axis=0, axis_index_groups=across, tiled=True
    )
    kv_all = lax.all_to_all(
        jnp.broadcast_to(column[None], (stripes,) + column.shape),
        "sp",
        split_axis=0,
        concat_axis=0,
        axis_index_groups=within,
        tiled=True,
    )
    query_send = jnp.transpose(
        queries.reshape(stripes, sub, KV_HEADS, group * HD), (2, 0, 1, 3)
    ).reshape(sp_count, sub, group * HD)
    query_got = lax.all_to_all(query_send, "sp", split_axis=0, concat_axis=0, tiled=True)
    extra_all = jnp.transpose(kv_all[:, :, tok:, :], (1, 0, 2, 3)).reshape(sp_count, 16, tok)
    extra_all = extra_all.astype(jnp.float32)
    boundary = jnp.sum((extra_all[:, 3 * group, :] < 0.5).astype(jnp.int32)).reshape(1)
    gates = extra_all[:, :group] + extra_all[:, group:2 * group] + extra_all[:, 2 * group:3 * group]
    gates = jnp.transpose(gates.reshape(tiles, blocks, group, tok), (0, 2, 1, 3))
    gates = jnp.transpose(gates.reshape(tiles, group, span // width, 1, width), (0, 2, 1, 3, 4))
    gates = gates.reshape(-1, group, 1, width)
    mixed = pl.pallas_call(
        functools.partial(attend_kernel, sub, span, width),
        grid=(tiles,),
        in_specs=[
            pl.BlockSpec(memory_space=pltpu.SMEM),
            pl.BlockSpec((blocks, sub, group * HD), lambda i: (i, 0, 0)),
            pl.BlockSpec(kv_all.shape, lambda i: (0, 0, 0, 0)),
            pl.BlockSpec(gates.shape, lambda i: (0, 0, 0, 0)),
        ],
        out_specs=pl.BlockSpec((blocks, sub, group * HD), lambda i: (i, 0, 0)),
        out_shape=jax.ShapeDtypeStruct((sp_count, sub, group * HD), jnp.bfloat16),
        compiler_params=pltpu.CompilerParams(vmem_limit_bytes=48 * 1024 * 1024),
        name="attend",
    )(boundary, query_got, kv_all, gates)
    back = lax.all_to_all(mixed, "sp", split_axis=0, concat_axis=0, tiled=True)
    attended = jnp.transpose(
        back.reshape(KV_HEADS, stripes, sub, group * HD), (1, 2, 0, 3)
    ).reshape(tok, QUERY_HEAD_COUNT * HD)
    hidden = (
        stream.astype(jnp.float32)
        + jnp.dot(attended, out_weight, preferred_element_type=jnp.float32)
    ).astype(jnp.bfloat16)
    hidden_f = hidden.astype(jnp.float32)
    normed = (
        hidden_f
        * lax.rsqrt(jnp.mean(hidden_f * hidden_f, axis=-1, keepdims=True) + EPS)
        * norm_gain
    ).astype(jnp.bfloat16)
    experts_total = sp_count
    capacity = max(2, 2 * tok * TOP // experts_total)
    slots = experts_total * capacity
    flat = routes.reshape(-1)
    hits = (flat[:, None] == jnp.arange(experts_total, dtype=jnp.int32)[None, :]).astype(jnp.int32)
    slot_index = jnp.sum(jnp.cumsum(hits, axis=0) * hits, axis=1) - 1
    target = (flat * capacity + slot_index).reshape(tok, TOP)
    line = jnp.arange(slots, dtype=jnp.int32)
    placed = sum(
        (line[:, None] == target[:, k][None, :]).astype(jnp.bfloat16) for k in range(TOP)
    )
    outgoing = jnp.dot(placed, normed, preferred_element_type=jnp.float32).astype(jnp.bfloat16)
    arrived = lax.all_to_all(
        outgoing.reshape(experts_total, capacity, -1), "sp", split_axis=0, concat_axis=0, tiled=True
    ).reshape(slots, -1)
    gate = jnp.dot(arrived, expert_gate[0], preferred_element_type=jnp.float32)
    upper = jnp.dot(arrived, expert_up[0], preferred_element_type=jnp.float32)
    inner = (jax.nn.silu(gate) * upper).astype(jnp.bfloat16)
    answer = jnp.dot(inner, expert_down[0], preferred_element_type=jnp.float32).astype(jnp.bfloat16)
    returned = lax.all_to_all(
        answer.reshape(sp_count, capacity, -1), "sp", split_axis=0, concat_axis=0, tiled=True
    ).reshape(slots, -1)
    share = sum(
        jnp.where(line[None, :] == target[:, k][:, None], route_weights[:, k][:, None], 0.0)
        for k in range(TOP)
    )
    share_high = lax.reduce_precision(share, 8, 7)
    share_low = (share - share_high).astype(jnp.bfloat16)
    routed = jnp.dot(
        share_high.astype(jnp.bfloat16), returned, preferred_element_type=jnp.float32
    ) + jnp.dot(share_low, returned, preferred_element_type=jnp.float32)
    return (hidden_f + routed).astype(jnp.bfloat16)


def solution(mesh):
    sp_count, tp_count = mesh.shape["sp"], mesh.shape["tp"]
    fast = tp_count == 1 and sp_count % 32 == 0
    return jax.shard_map(
        fast_shards if fast else shards,
        mesh=mesh,
        in_specs=(
            P("sp", "tp"),
            P("sp", "tp"),
            P("sp", "tp"),
            P("sp", "tp"),
            P("sp"),
            P(("sp", "tp"), None),
            P(),
            P(),
            P(("sp", "tp"), None),
            P(("sp", "tp"), None),
            P("sp", None, "tp"),
            P("sp", None, "tp"),
            P("sp", "tp", None),
        ),
        out_specs=P(("sp", "tp"), None),
        check_vma=False,
    )
```
